32 devices in a mesh: ep: 4 (over y, x), tp: 8 (over z, core).
Axes of the slice: x: 2, y: 2, z: 4, core: 2. Of those that a mesh axis runs over, the one named last changes fastest.
Arguments:
- pool_input: bfloat16 [4096, 1024], P('ep', 'tp'), may hold values from -6 to 6
- pool_gain: float32 [1024], P('tp'), may hold values from 0.1 to 1.9
- mix_weight: bfloat16 [1024, 2048], P('tp'), may hold values from -0.1875 to 0.1875
- moe_input: bfloat16 [8192, 2048], P(('ep', 'tp')), may hold values from -6 to 6
- moe_gain: float32 [2048], replicated, may hold values from 0.1 to 1.9
- expert_ids: int32 [8192, 2], P(('ep', 'tp')), may hold values from 0 to 15, as said below
- route_weight: float32 [8192, 2], P(('ep', 'tp')), may hold values from 0.2 to 1
- gate_weight: bfloat16 [16, 2048, 1024], P('ep', None, 'tp'), may hold values from -0.125 to 0.125
- up_weight: bfloat16 [16, 2048, 1024], P('ep', None, 'tp'), may hold values from -0.125 to 0.125
- down_weight: bfloat16 [16, 2048, 1024], P('ep', None, 'tp'), may hold values from -0.1875 to 0.1875
Outputs:
- mixed_out: bfloat16 [4096, 2048], P(('ep', 'tp'))
- moe_out: bfloat16 [8192, 2048], P(('ep', 'tp'))
The draws below stay inside these ranges and needn't reach their ends.
Inputs may be any that keep to these rules, and one draw needn't show every extreme that they name: `expert_ids`: each row names 2 different experts of one group of 4 consecutive experts. In each aligned block of 256 rows (the rows of one device) no expert is named by more than 48 rows, and some expert is named by exactly 48 rows.
All inputs are finite; a program needn't handle non-finite values.
Results may differ from the reference program's by a relative error of at most 0.012.
Values may be sent and summed in bfloat16 or wider, within the bound.
A program may use at most 128 MiB of HBM per device.

```python
import math
import jax
import jax.numpy as jnp
from jax import lax

D = 2048
PW = 1024
GROUP_CH = 256
FF = 1024
EXPERTS = 16
GROUP_EXP = 4
TOP = 2
ROWS_B = 256
CAP = 48
TOK_A = 4096
TOK_B = 8192


def block_routes(block_key):
    subkeys = jax.random.split(block_key, 5)
    remaining = ROWS_B - 2 * CAP
    share_base = remaining // 3
    spread = share_base // 4
    first_shift = jax.random.randint(subkeys[0], (), -spread, spread + 1)
    second_shift = jax.random.randint(subkeys[1], (), -spread, spread + 1)
    others = jnp.stack([share_base + first_shift, share_base + second_shift, remaining - 2 * share_base - first_shift - second_shift]).astype(jnp.int32)
    largest = jax.random.randint(subkeys[2], (), 0, 4)
    group_range = jnp.arange(4, dtype=jnp.int32)
    other_index = jnp.clip(group_range - (group_range > largest).astype(jnp.int32), 0, 2)
    quotas = jnp.where(group_range == largest, 2 * CAP, others[other_index]).astype(jnp.int32)
    group_ends = jnp.cumsum(quotas)
    position = jnp.arange(ROWS_B, dtype=jnp.int32)
    member = jnp.sum((position[:, None] >= group_ends[None, :]).astype(jnp.int32), axis=1)
    within = position - (group_ends - quotas)[member]
    leading = within % 4
    trailing = (within + 1 + within // 4 % 3) % 4
    relabel = jax.random.permutation(subkeys[3], 4).astype(jnp.int32)
    routes = jnp.stack([member * GROUP_EXP + relabel[leading], member * GROUP_EXP + relabel[trailing]], axis=1)
    return routes[jax.random.permutation(subkeys[4], ROWS_B)].astype(jnp.int32)


def draw_expert_ids(key, part):
    block_keys = jax.random.split(jax.random.fold_in(key, 7), TOK_B // ROWS_B)
    return jax.vmap(block_routes)(block_keys).reshape(TOK_B, 2)


def level_of(stream_key, shape, cuts, least, top_value):
    def one(dim, shards_of):
        heights = jax.random.uniform(jax.random.fold_in(jax.random.fold_in(stream_key, 6), dim), (shards_of,), jnp.float32, least / len(cuts), top_value / len(cuts))
        return jnp.repeat(jnp.exp(heights), shape[dim] // shards_of).reshape((-1,) + (1,) * (len(shape) - dim - 1))

    loudness = one(*cuts[0])
    for cut in cuts[1:]:
        loudness = loudness * one(*cut)
    return loudness


def normal_values(stream_key, dims, deviation, limit, cuts=(), kind=jnp.bfloat16):
    result = deviation * jax.random.normal(stream_key, dims, jnp.float32)
    if cuts:
        result = result * level_of(stream_key, dims, cuts, -0.22, 0.18)
    return jnp.clip(result, -limit, limit).astype(kind)


def setup_inputs(seed: int = 0) -> dict:
    key_of = jax.random.split(jax.random.key(seed), 11)
    pool_input = normal_values(key_of[0], (TOK_A, PW), 1.0, 6.0, ((0, 4), (1, 8)))
    pool_gain = jnp.clip(1.0 + 0.18 * jax.random.normal(key_of[1], (PW,), jnp.float32), 0.1, 1.9)
    mix_weight = normal_values(key_of[2], (PW, D), PW ** -0.5, 0.1875, ((0, 8),))
    moe_input = normal_values(key_of[3], (TOK_B, D), 1.0, 6.0, ((0, 32),))
    moe_gain = jnp.clip(1.0 + 0.18 * jax.random.normal(key_of[4], (D,), jnp.float32), 0.1, 1.9)
    expert_ids = draw_expert_ids(jax.random.fold_in(key_of[10], 71), 0)
    route_weight = jnp.clip(jnp.exp(math.log(1.0) - 1.609438 * jax.random.uniform(key_of[6], (TOK_B, TOP), jnp.float32) ** level_of(key_of[6], (TOK_B, TOP), ((0, 32),), -0.2, 0.2)), 0.2, 1.0)
    gate_weight = normal_values(key_of[7], (EXPERTS, D, FF), D ** -0.5, 0.125, ((0, 4), (2, 8)))
    up_weight = normal_values(key_of[8], (EXPERTS, D, FF), D ** -0.5, 0.125, ((0, 4), (2, 8)))
    down_weight = normal_values(key_of[9], (EXPERTS, D, FF), FF ** -0.5, 0.1875, ((0, 4), (2, 8)))
    return dict(pool_input=pool_input, pool_gain=pool_gain, mix_weight=mix_weight, moe_input=moe_input, moe_gain=moe_gain, expert_ids=expert_ids, route_weight=route_weight, gate_weight=gate_weight, up_weight=up_weight, down_weight=down_weight)


eps_norm = 1e-06

def reference(pool_input, pool_gain, mix_weight, moe_input, moe_gain, expert_ids, route_weight, gate_weight, up_weight, down_weight):
    values = pool_input.astype(jnp.float32)
    length = values.shape[0]
    running = jnp.concatenate([jnp.zeros((1, PW), jnp.float32), jnp.cumsum(values, axis=0)], axis=0)
    position = jnp.arange(length, dtype=jnp.int32)
    pieces = []
    for index_group in range(4):
        window = 2 ** (index_group + 1)
        begins = jnp.maximum(position + 1 - window, 0)
        counted = (position + 1 - begins).astype(jnp.float32)
        column = running[:, index_group * GROUP_CH:(index_group + 1) * GROUP_CH]
        pieces.append((column[1:] - column[begins]) / counted[:, None])
    pooled = ((jnp.concatenate(pieces, axis=1) - values) * pool_gain).astype(jnp.bfloat16)
    mixed_out = jnp.dot(pooled, mix_weight, preferred_element_type=jnp.float32).astype(jnp.bfloat16)
    inputs = moe_input.astype(jnp.float32)
    scale_rows = lax.rsqrt(lax.optimization_barrier(jnp.mean(inputs * inputs, axis=-1, keepdims=True)) + eps_norm)
    normed = (inputs * scale_rows * moe_gain).astype(jnp.bfloat16)
    blocks = TOK_B // ROWS_B
    chosen = expert_ids.reshape(blocks, ROWS_B * TOP)
    marked = (chosen[:, :, None] == jnp.arange(EXPERTS, dtype=jnp.int32)[None, None, :]).astype(jnp.int32)
    ranked = lax.optimization_barrier(jnp.sum((jnp.cumsum(marked, axis=1) - marked) * marked, axis=2)).astype(jnp.int32)
    owner_row = (jnp.arange(ROWS_B * TOP, dtype=jnp.int32)[None, :] // TOP + jnp.arange(blocks, dtype=jnp.int32)[:, None] * ROWS_B).astype(jnp.int32)
    block_ids = jnp.broadcast_to(jnp.arange(blocks, dtype=jnp.int32)[:, None], chosen.shape)
    source = jnp.full((EXPERTS, blocks, CAP), TOK_B, jnp.int32).at[chosen, block_ids, ranked].set(owner_row)
    padded = jnp.concatenate([normed, jnp.zeros((1, D), jnp.bfloat16)], axis=0)

    def expert_pass(operands):
        indices, gate_mat, up_mat, down_mat = operands
        gathered = padded[indices.reshape(-1)]
        gate_part = jnp.dot(gathered, gate_mat, preferred_element_type=jnp.float32)
        upward = jnp.dot(gathered, up_mat, preferred_element_type=jnp.float32)
        hidden = (jax.nn.silu(gate_part) * upward).astype(jnp.bfloat16)
        return jnp.dot(hidden, jnp.transpose(down_mat), preferred_element_type=jnp.float32).astype(jnp.bfloat16)
    results = lax.map(expert_pass, (source, gate_weight, up_weight, down_weight))
    flat_index = (chosen * (blocks * CAP) + block_ids * CAP + ranked).astype(jnp.int32)
    picked = results.reshape(EXPERTS * blocks * CAP, D)[flat_index.reshape(-1)].astype(jnp.float32)
    picked = picked.reshape(TOK_B, TOP, D)
    moe_out = lax.optimization_barrier(jnp.sum(picked * route_weight[:, :, None], axis=1)).astype(jnp.bfloat16)
    return (mixed_out, moe_out)
```

```python
import jax
import jax.numpy as jnp
from jax import lax
from jax.sharding import PartitionSpec as P

GROUP_CH = 256
EXPERTS = 16
GROUP_EXP = 4
TOP = 2
CAP = 48


eps_norm = 1e-06


def from_behind(shard, axis, by):
    peers = lax.axis_size(axis)
    pairs = [(i, i + by) for i in range(peers) if 0 <= i + by < peers]
    return lax.ppermute(shard, axis, pairs)


def window_sums(extended, row_count):
    level_sum = extended
    stride = 1
    outputs = []
    for doubling in range(4):
        level_sum = level_sum[stride:] + level_sum[:-stride]
        stride = stride * 2
        outputs.append(level_sum[level_sum.shape[0] - row_count :])
    return outputs


def pool_mixer(pool_input, pool_gain):
    row_count, channels = pool_input.shape
    carried = from_behind(pool_input[row_count - 15 :], "ep", 1)
    extended = jnp.concatenate([carried, pool_input], axis=0).astype(jnp.float32)
    window_list = window_sums(extended, row_count)
    channel_ids = lax.axis_index("tp") * channels + lax.iota(jnp.int32, channels)
    group_ids = channel_ids // GROUP_CH
    position = lax.axis_index("ep") * row_count + lax.iota(jnp.int32, row_count)
    summed = jnp.zeros((row_count, channels), jnp.float32)
    widths = jnp.zeros((channels,), jnp.int32)
    for index_group in range(4):
        inside = group_ids == index_group
        summed = jnp.where(inside[None, :], window_list[index_group], summed)
        widths = jnp.where(inside, 2 ** (index_group + 1), widths)
    counted = jnp.minimum(position[:, None] + 1, widths[None, :]).astype(jnp.float32)
    values = extended[15:]
    return ((summed / counted - values) * pool_gain).astype(jnp.bfloat16)


def dispatch_plan(expert_ids, route_weight, ep_size):
    local_experts = EXPERTS // ep_size
    share = TOP if local_experts % GROUP_EXP == 0 else 1
    capacity = local_experts * CAP // share
    owners = expert_ids // local_experts
    ep_index = lax.iota(jnp.int32, ep_size)
    member = jnp.any(owners[:, :, None] == ep_index[None, None, :], axis=1)
    counts = member.astype(jnp.int32)
    rank = jnp.cumsum(counts, axis=0) - counts
    slot = jnp.where(member, rank, -1).T
    placing = slot[:, None, :] == lax.iota(jnp.int32, capacity)[None, :, None]
    dense_weight = jnp.sum(
        jnp.where(
            expert_ids[:, :, None] == lax.iota(jnp.int32, EXPERTS)[None, None, :],
            route_weight[:, :, None],
            0.0,
        ),
        axis=1,
    )
    dense_weight = dense_weight.reshape(-1, ep_size, local_experts)
    slot_weight = jnp.einsum(
        "ecn,nej->ecj",
        placing.astype(jnp.float32),
        dense_weight,
        precision=lax.Precision.HIGHEST,
    )
    return placing.astype(jnp.bfloat16).reshape(ep_size * capacity, -1), slot_weight, capacity


def body(
    pool_input,
    pool_gain,
    mix_weight,
    moe_input,
    moe_gain,
    expert_ids,
    route_weight,
    gate_weight,
    up_weight,
    down_weight,
):
    pooled = pool_mixer(pool_input, pool_gain)
    regrouped = lax.all_to_all(pooled, "tp", split_axis=0, concat_axis=1, tiled=True)
    mixed_sum = jnp.dot(
        regrouped,
        lax.all_gather(mix_weight, "tp", axis=0, tiled=True),
        preferred_element_type=jnp.float32,
    )
    mixed_out = mixed_sum.astype(jnp.bfloat16)
    inputs = moe_input.astype(jnp.float32)
    scale_rows = lax.rsqrt(jnp.mean(inputs * inputs, axis=-1, keepdims=True) + eps_norm)
    normed = (inputs * scale_rows * moe_gain).astype(jnp.bfloat16)
    ep_size = lax.axis_size("ep")
    placing, slot_weight, capacity = dispatch_plan(expert_ids, route_weight, ep_size)
    outgoing = jnp.dot(placing, normed, preferred_element_type=jnp.float32).astype(jnp.bfloat16)
    arrived = lax.all_to_all(outgoing, "ep", split_axis=0, concat_axis=0, tiled=True)
    weights = lax.all_to_all(slot_weight, "ep", split_axis=0, concat_axis=0, tiled=True)
    weights = weights.reshape(ep_size * capacity, -1)
    tokens = lax.all_gather(arrived, "tp", axis=0, tiled=True)
    weights = lax.all_gather(weights, "tp", axis=0, tiled=True)
    gate_part = jnp.einsum("nd,edf->enf", tokens, gate_weight, preferred_element_type=jnp.float32)
    upward = jnp.einsum("nd,edf->enf", tokens, up_weight, preferred_element_type=jnp.float32)
    hidden = (jax.nn.silu(gate_part) * upward * weights.T[:, :, None]).astype(jnp.bfloat16)
    partial = jnp.einsum("enf,edf->nd", hidden, down_weight, preferred_element_type=jnp.float32)
    reduced = lax.psum_scatter(
        partial.astype(jnp.bfloat16), "tp", scatter_dimension=0, tiled=True
    )
    returned = lax.all_to_all(reduced, "ep", split_axis=0, concat_axis=0, tiled=True)
    combined = lax.dot_general(
        placing, returned, (((0,), (0,)), ((), ())), preferred_element_type=jnp.float32
    )
    moe_out = combined.astype(jnp.bfloat16)
    return (mixed_out, moe_out)


def solution(mesh):
    return jax.shard_map(
        body,
        mesh=mesh,
        in_specs=(
            P("ep", "tp"),
            P("tp"),
            P("tp", None),
            P(("ep", "tp"), None),
            P(),
            P(("ep", "tp"), None),
            P(("ep", "tp"), None),
            P("ep", None, "tp"),
            P("ep", None, "tp"),
            P("ep", None, "tp"),
        ),
        out_specs=(P(("ep", "tp"), None), P(("ep", "tp"), None)),
        check_vma=False,
    )
```

```python
import jax
import jax.numpy as jnp
from jax import lax
from jax.sharding import PartitionSpec as P

GROUP_CH = 256
EXPERTS = 16
GROUP_EXP = 4
TOP = 2
CAP = 48
CHUNKS = 2


eps_norm = 1e-06


def from_behind(shard, axis, by):
    peers = lax.axis_size(axis)
    pairs = [(i, i + by) for i in range(peers) if 0 <= i + by < peers]
    return lax.ppermute(shard, axis, pairs)


def window_sums(extended, row_count):
    level_sum = extended
    stride = 1
    outputs = []
    for doubling in range(4):
        level_sum = level_sum[stride:] + level_sum[:-stride]
        stride = stride * 2
        outputs.append(level_sum[level_sum.shape[0] - row_count :])
    return outputs


def pool_mixer(pool_input, pool_gain):
    row_count, channels = pool_input.shape
    carried = from_behind(pool_input[row_count - 15 :], "ep", 1)
    extended = jnp.concatenate([carried, pool_input], axis=0).astype(jnp.float32)
    window_list = window_sums(extended, row_count)
    channel_ids = lax.axis_index("tp") * channels + lax.iota(jnp.int32, channels)
    group_ids = channel_ids // GROUP_CH
    position = lax.axis_index("ep") * row_count + lax.iota(jnp.int32, row_count)
    summed = jnp.zeros((row_count, channels), jnp.float32)
    widths = jnp.zeros((channels,), jnp.int32)
    for index_group in range(4):
        inside = group_ids == index_group
        summed = jnp.where(inside[None, :], window_list[index_group], summed)
        widths = jnp.where(inside, 2 ** (index_group + 1), widths)
    counted = jnp.minimum(position[:, None] + 1, widths[None, :]).astype(jnp.float32)
    values = extended[15:]
    return ((summed / counted - values) * pool_gain).astype(jnp.bfloat16)


def dispatch_plan(expert_ids, route_weight, ep_size):
    local_experts = EXPERTS // ep_size
    share = TOP if local_experts % GROUP_EXP == 0 else 1
    capacity = local_experts * CAP // share
    owners = expert_ids // local_experts
    ep_index = lax.iota(jnp.int32, ep_size)
    member = jnp.any(owners[:, :, None] == ep_index[None, None, :], axis=1)
    counts = member.astype(jnp.int32)
    rank = jnp.cumsum(counts, axis=0) - counts
    slot = jnp.where(member, rank, -1).T
    placing = slot[:, None, :] == lax.iota(jnp.int32, capacity)[None, :, None]
    dense_weight = jnp.sum(
        jnp.where(
            expert_ids[:, :, None] == lax.iota(jnp.int32, EXPERTS)[None, None, :],
            route_weight[:, :, None],
            0.0,
        ),
        axis=1,
    )
    dense_weight = dense_weight.reshape(-1, ep_size, local_experts)
    slot_weight = jnp.einsum(
        "ecn,nej->ecj",
        placing.astype(jnp.float32),
        dense_weight,
        precision=lax.Precision.HIGHEST,
    )
    return placing.astype(jnp.bfloat16).reshape(ep_size * capacity, -1), slot_weight, capacity


def body(
    pool_input,
    pool_gain,
    mix_weight,
    moe_input,
    moe_gain,
    expert_ids,
    route_weight,
    gate_weight,
    up_weight,
    down_weight,
):
    pooled = pool_mixer(pool_input, pool_gain)
    ep_size = lax.axis_size("ep")
    out_columns = mix_weight.shape[1] // ep_size
    mix_columns = lax.dynamic_slice_in_dim(
        mix_weight, lax.axis_index("ep") * out_columns, out_columns, axis=1
    )
    mix_columns = lax.all_gather(mix_columns, "tp", axis=0, tiled=True)
    inputs = moe_input.astype(jnp.float32)
    scale_rows = lax.rsqrt(jnp.mean(inputs * inputs, axis=-1, keepdims=True) + eps_norm)
    normed = (inputs * scale_rows * moe_gain).astype(jnp.bfloat16)
    placing, slot_weight, capacity = dispatch_plan(expert_ids, route_weight, ep_size)
    rows = capacity // CHUNKS
    arrived_list = []
    placing_list = []
    for chunk in range(CHUNKS):
        chunk_placing = placing.reshape(ep_size, capacity, -1)[:, chunk * rows : (chunk + 1) * rows]
        chunk_placing = chunk_placing.reshape(ep_size * rows, -1)
        outgoing = jnp.dot(chunk_placing, normed, preferred_element_type=jnp.float32)
        outgoing = outgoing.astype(jnp.bfloat16)
        placing_list.append(chunk_placing)
        arrived_list.append(
            lax.all_to_all(outgoing, "ep", split_axis=0, concat_axis=0, tiled=True)
        )
    arrived_list[0], mix_columns = lax.optimization_barrier((arrived_list[0], mix_columns))
    weights = lax.all_to_all(slot_weight, "ep", split_axis=0, concat_axis=0, tiled=True)
    weights = lax.all_gather(weights, "tp", axis=0, tiled=True)
    combined = jnp.zeros(normed.shape, jnp.float32)
    for chunk in range(CHUNKS):
        tokens = lax.all_gather(arrived_list[chunk], "tp", axis=0, tiled=True)
        scales = weights[:, chunk * rows : (chunk + 1) * rows].reshape(tokens.shape[0], -1)
        gate_part = jnp.einsum(
            "nd,edf->enf", tokens, gate_weight, preferred_element_type=jnp.float32
        )
        upward = jnp.einsum("nd,edf->enf", tokens, up_weight, preferred_element_type=jnp.float32)
        hidden = (jax.nn.silu(gate_part) * upward * scales.T[:, :, None]).astype(jnp.bfloat16)
        partial = jnp.einsum("enf,edf->nd", hidden, down_weight, preferred_element_type=jnp.float32)
        reduced = lax.psum_scatter(
            partial.astype(jnp.bfloat16), "tp", scatter_dimension=0, tiled=True
        )
        returned = lax.all_to_all(reduced, "ep", split_axis=0, concat_axis=0, tiled=True)
        combined = combined + lax.dot_general(
            placing_list[chunk],
            returned,
            (((0,), (0,)), ((), ())),
            preferred_element_type=jnp.float32,
        )
    moe_out = combined.astype(jnp.bfloat16)
    regrouped = lax.all_to_all(pooled, "tp", split_axis=0, concat_axis=1, tiled=True)
    half = regrouped.shape[1] // 2
    mixed_sum = 0.0
    for part in range(2):
        section = slice(part * half, (part + 1) * half)
        pooled_rows = lax.all_gather(regrouped[:, section], "ep", axis=0, tiled=True)
        mixed_sum = mixed_sum + jnp.dot(
            pooled_rows, mix_columns[section], preferred_element_type=jnp.float32
        )
    mixed_out = lax.all_to_all(
        mixed_sum.astype(jnp.bfloat16), "ep", split_axis=0, concat_axis=1, tiled=True
    )
    return (mixed_out, moe_out)


def solution(mesh):
    return jax.shard_map(
        body,
        mesh=mesh,
        in_specs=(
            P("ep", "tp"),
            P("tp"),
            P("tp", None),
            P(("ep", "tp"), None),
            P(),
            P(("ep", "tp"), None),
            P(("ep", "tp"), None),
            P("ep", None, "tp"),
            P("ep", None, "tp"),
            P("ep", None, "tp"),
        ),
        out_specs=(P(("ep", "tp"), None), P(("ep", "tp"), None)),
        check_vma=False,
    )
```
